32 devices in a mesh: fs: 8 (over z, y), tp: 4 (over x, core).
Axes of the slice: x: 2, y: 2, z: 4, core: 2. Of those that a mesh axis runs over, the one named last changes fastest.
Arguments:
- tokens: bfloat16 [8192, 2048], P('fs', 'tp'), may hold values from -6 to 6
- norm_gain: float32 [2048], P('fs'), may hold values from 0.1 to 1.9
- up_master: float32 [2048, 8192], P('fs', 'tp'), may hold values from -0.125 to 0.125
- down_master: float32 [2048, 8192], P('fs', 'tp'), may hold values from -0.0625 to 0.0625
Outputs:
- up_weights: bfloat16 [2048, 8192], P(None, 'tp')
- down_weights: bfloat16 [8192, 2048], P('tp')
- mlp_out: bfloat16 [8192, 2048], P('fs', 'tp')
The draws below stay inside these ranges and needn't reach their ends.
All inputs are finite; a program needn't handle non-finite values.
Results may differ from the reference program's by a relative error of at most 0.014.
Values may be sent and summed in bfloat16 or wider, within the bound.
A program may use at most 128 MiB of HBM per device.

```python
import jax
import jax.numpy as jnp
from jax import lax

D = 2048
FF = 8192
TOKENS = 8192
N_TP = 4


def block_scale(key, extent, cuts, smallest, high):
    loudness = 1.0
    for axis_at, parts in cuts:
        draws = jax.random.uniform(jax.random.fold_in(jax.random.fold_in(key, 6), axis_at), (parts,), jnp.float32, smallest / len(cuts), high / len(cuts))
        loudness = loudness * jnp.repeat(jnp.exp(draws), extent[axis_at] // parts).reshape((-1,) + (1,) * (len(extent) - 1 - axis_at))
    return loudness


def bell_draw(stream_key, shape, width, limit, shards=(), held_as=jnp.bfloat16):
    result = jax.random.normal(stream_key, shape, jnp.float32) * width
    if len(shards) > 0:
        result = block_scale(stream_key, shape, shards, -0.22, 0.18) * result
    return jnp.clip(result, min=-limit, max=limit).astype(held_as)


def setup_inputs(seed: int = 0) -> dict:
    key_list = jax.random.split(jax.random.key(seed), 5)
    tokens = bell_draw(key_list[0], (TOKENS, D), 1.0, 6.0, ((0, 8), (1, 4)))
    norm_gain = jnp.clip(1.0 + 0.18 * jax.random.normal(key_list[1], (D,), jnp.float32), 0.1, 1.9)
    up_master = bell_draw(key_list[2], (D, FF), D ** -0.5, 0.125, ((0, 8), (1, 4)), jnp.float32)
    down_master = bell_draw(key_list[3], (D, FF), FF ** -0.5, 0.0625, ((0, 8), (1, 4)), jnp.float32)
    return {"tokens": tokens, "norm_gain": norm_gain, "up_master": up_master, "down_master": down_master}


norm_floor = 1e-06

def reference(tokens, norm_gain, up_master, down_master):
    up_weights = (norm_gain[:, None] * up_master).astype(jnp.bfloat16)
    down_weights = jnp.transpose(down_master).astype(jnp.bfloat16)
    widened = tokens.astype(jnp.float32)
    normed = (widened * lax.rsqrt(lax.optimization_barrier(jnp.mean(widened * widened, axis=-1, keepdims=True)) + norm_floor)).astype(jnp.bfloat16)
    preact = jnp.dot(normed, up_weights, preferred_element_type=jnp.float32)
    hidden = jnp.square(jax.nn.relu(preact)).astype(jnp.bfloat16)
    block = FF // N_TP
    hidden_blocks = jnp.transpose(hidden.reshape(hidden.shape[0], N_TP, block), (1, 0, 2))
    down_blocks = down_weights.reshape(N_TP, block, D)

    def accumulate(total, pieces):
        partial_value = jnp.dot(pieces[0], pieces[1], preferred_element_type=jnp.float32).astype(jnp.bfloat16)
        partial_value = lax.optimization_barrier(partial_value)
        return (total + partial_value.astype(jnp.float32), None)
    start_total = jnp.zeros((hidden.shape[0], D), jnp.float32)
    total, unused = lax.scan(accumulate, start_total, (hidden_blocks, down_blocks))
    return (up_weights, down_weights, total.astype(jnp.bfloat16))
```

```python
import functools

import jax
import jax.numpy as jnp
from jax import lax
from jax.experimental import pallas as pl
from jax.experimental.pallas import tpu as pltpu
from jax.sharding import PartitionSpec as P

norm_floor = 1e-06
MESH = pl.DeviceIdType.MESH


def grid_of(n):
    ny = max(d for d in range(1, n + 1) if n % d == 0 and d * d <= n)
    return n // ny, ny


def position_of(f, nz, ny):
    if ny == 1:
        return f
    z, y = lax.div(f, ny), lax.rem(f, ny)
    tail = lax.div(y + (ny - 1), ny)
    k = nz - 1 - z
    odd = lax.rem(k, 2)
    r = (1 - odd) * (y - 1) + odd * (ny - 1 - y)
    return (1 - tail) * z + tail * (nz + k * (ny - 1) + r)


def index_at(p, nz, ny):
    if ny == 1:
        return p
    tail = lax.div(lax.div(p, nz) + (ny - 2), ny - 1)
    q = tail * (p - nz)
    k = lax.div(q, ny - 1)
    r = lax.rem(q, ny - 1)
    odd = lax.rem(k, 2)
    z = (1 - tail) * p + tail * (nz - 1 - k)
    y = tail * ((1 - odd) * (1 + r) + odd * (ny - 1 - r))
    return z * ny + y


def send_list(n):
    hops = n // 2
    split = n % 2 == 0

    def pieces(a, h):
        return [(a, h, 0)] if split and h == hops - 1 else [(a, h, 0), (a, h, 1)]

    ups = [p for h in range(1, hops) for p in pieces("u", h)]
    downs = [p for h in range(1, hops) for p in pieces("d", h)]
    own_u, own_d = pieces("u", 0), pieces("d", 0)
    return own_u + own_d[:1] + ups + own_d[1:] + downs


def gather_kernel(n_fs, n_tp, tokens, up_l, dn_l, up_w, dn_w, recv, x, hid, part, loc_sem, tok_s, tok_r, ring_s, ring_r, rs_s, rs_r):
    nz, ny = grid_of(n_fs)
    me_f, me_t = lax.axis_index("fs"), lax.axis_index("tp")
    pos = position_of(me_f, nz, ny)
    T, Dk = tokens.shape
    R, F = up_l.shape
    D = n_fs * R
    split_cols = (R // 2) % 128 == 0
    W = R // 2 if split_cols else R

    def at(offset):
        return index_at(lax.rem(pos + offset + n_fs, n_fs), nz, ny)

    right, left = at(1), at(-1)

    def tp_peer(k):
        return lax.rem(me_t + k, n_tp)

    barrier = pltpu.get_barrier_semaphore()
    for f in (right, left):
        pl.semaphore_signal(barrier, inc=1, device_id={"fs": f, "tp": me_t}, device_id_type=MESH)
    for k in range(1, n_tp):
        pl.semaphore_signal(barrier, inc=1, device_id={"fs": me_f, "tp": tp_peer(k)}, device_id_type=MESH)

    def up_piece(f, h):
        return up_w.at[pl.ds(pl.multiple_of(f * R + h * (R // 2), R // 2), R // 2), :]

    def dn_piece(f, h):
        if split_cols:
            return dn_w.at[:, pl.ds(pl.multiple_of(f * R + h * (R // 2), R // 2), R // 2)]
        return dn_w.at[pl.ds(h * (F // 2), F // 2), pl.ds(pl.multiple_of(f * R, R), R)]

    def tok_cols(t):
        return x.at[:, pl.ds(pl.multiple_of(t * Dk, Dk), Dk)]

    own = [
        pltpu.make_async_copy(up_l, up_w.at[pl.ds(pl.multiple_of(me_f * R, R), R), :], loc_sem.at[0]),
        pltpu.make_async_copy(dn_l, dn_w.at[:, pl.ds(pl.multiple_of(me_f * R, R), R)], loc_sem.at[1]),
        pltpu.make_async_copy(tokens, tok_cols(me_t), loc_sem.at[2]),
    ]
    for c in own:
        c.start()
    pl.semaphore_wait(barrier, n_tp + 1)

    order = send_list(n_fs)
    S = len(order)

    def ring_copy(s, d):
        a, hop, second = order[s]
        half = second if d == 0 else 1 - second
        f = at(-hop if d == 0 else hop)
        ref = up_piece(f, half) if a == "u" else dn_piece(f, half)
        return pltpu.make_async_remote_copy(
            src_ref=ref, dst_ref=ref, send_sem=ring_s.at[d, s], recv_sem=ring_r.at[d, s],
            device_id={"fs": right if d == 0 else left, "tp": me_t}, device_id_type=MESH,
        )

    def arrival(s, d):
        a, hop, second = order[s]
        half = second if d == 0 else 1 - second
        f = at(-(hop + 1) if d == 0 else hop + 1)
        return f, half, (up_piece(f, half) if a == "u" else dn_piece(f, half))

    def wait_arrival(s, d):
        f, half, ref = arrival(s, d)
        pltpu.make_async_remote_copy(
            src_ref=ref, dst_ref=ref, send_sem=ring_s.at[d, s], recv_sem=ring_r.at[d, s],
            device_id={"fs": right if d == 0 else left, "tp": me_t}, device_id_type=MESH,
        ).wait_recv()

    needs = [-1 if hop == 0 else order.index((a, hop - 1, second)) for a, hop, second in order]
    issued = [0]

    def issue(upto):
        while issued[0] < S and needs[issued[0]] <= upto:
            if upto < 0 and issued[0] >= 3:
                break
            for d in range(2):
                ring_copy(issued[0], d).start()
            issued[0] += 1

    own[0].wait()
    for d in range(2):
        ring_copy(0, d).start()
        ring_copy(1, d).start()
    own[2].wait()

    def token_copy(k):
        return pltpu.make_async_remote_copy(
            src_ref=tok_cols(me_t), dst_ref=tok_cols(me_t), send_sem=tok_s.at[k], recv_sem=tok_r.at[k],
            device_id={"fs": me_f, "tp": tp_peer(k)}, device_id_type=MESH,
        )

    for k in range(1, n_tp):
        token_copy(k).start()
    own[1].wait()
    issued[0] = 2
    issue(-1)

    def normalise():
        for k in range(1, n_tp):
            src = lax.rem(me_t - k + n_tp, n_tp)
            pltpu.make_async_remote_copy(
                src_ref=tok_cols(src), dst_ref=tok_cols(src), send_sem=tok_s.at[k], recv_sem=tok_r.at[k],
                device_id={"fs": me_f, "tp": tp_peer(k)}, device_id_type=MESH,
            ).wait_recv()
            token_copy(k).wait_send()
        rows = 64

        @pl.loop(0, T // rows)
        def _(i):
            r = pl.ds(pl.multiple_of(i * rows, rows), rows)
            v = x[r, :].astype(jnp.float32)
            x[r, :] = (v * lax.rsqrt(jnp.mean(v * v, axis=-1, keepdims=True) + norm_floor)).astype(jnp.bfloat16)

    def make_hidden():
        width = 256

        @pl.loop(0, F // width)
        def _(i):
            c = pl.ds(pl.multiple_of(i * width, width), width)
            pre = jnp.dot(x[...], up_w[:, c], preferred_element_type=jnp.float32)
            hid[:, c] = jnp.square(jnp.maximum(pre, 0.0)).astype(jnp.bfloat16)

    per_owner = Dk // W

    def part_copy(q):
        owner = lax.div(q, per_owner)
        local = lax.rem(q, per_owner)
        return owner, pltpu.make_async_remote_copy(
            src_ref=part.at[q],
            dst_ref=recv.at[me_t, :, pl.ds(pl.multiple_of(local * W, W), W)],
            send_sem=rs_s.at[q], recv_sem=rs_r.at[me_t, local],
            device_id={"fs": me_f, "tp": owner}, device_id_type=MESH,
        )

    def do_part(q):
        rows = T // 2
        owner, copy = part_copy(q)
        c = pl.ds(pl.multiple_of(q * W, W), W)

        @pl.loop(0, 2)
        def _(i):
            r = pl.ds(pl.multiple_of(i * rows, rows), rows)
            part[q, r, :] = jnp.dot(hid[r, :], dn_w[:, c], preferred_element_type=jnp.float32).astype(jnp.bfloat16)

        @pl.when(owner != me_t)
        def _():
            copy.start()

    ready = [me_f * (R // W) + h for h in range(R // W)]
    last_up = max(s for s in range(S) if order[s][0] == "u")
    norm_at = max(0, last_up - 2)
    for s in range(S):
        for d in range(2):
            wait_arrival(s, d)
        issue(s)
        if order[s][0] == "d" and split_cols:
            for d in range(2):
                f, half, _ = arrival(s, d)
                ready.append(f * 2 + half)
        if s == norm_at:
            normalise()
        if s == last_up:
            make_hidden()
        if s >= last_up:
            for q in ready:
                do_part(q)
            ready = []
    if not split_cols:
        @pl.loop(0, n_fs)
        def _(q):
            @pl.when(q != me_f)
            def _():
                do_part(q)

    keep = pl.ds(pl.multiple_of(0, W), W)

    @pl.loop(0, per_owner)
    def _(local):
        cols = pl.ds(pl.multiple_of(local * W, W), W)
        recv[me_t, :, cols] = part[me_t * per_owner + local]

    for d in range(2):
        for s in range(S):
            ring_copy(s, d).wait_send()

    @pl.loop(0, D // W)
    def _(q):
        owner, copy = part_copy(q)

        @pl.when(owner != me_t)
        def _():
            copy.wait_send()

    for k in range(1, n_tp):
        src = tp_peer(k)
        for local in range(per_owner):
            ref = recv.at[src, :, pl.ds(local * W, W)]
            pltpu.make_async_remote_copy(
                src_ref=ref, dst_ref=ref, send_sem=rs_s.at[0], recv_sem=rs_r.at[src, local],
                device_id={"fs": me_f, "tp": src}, device_id_type=MESH,
            ).wait_recv()


def finish_kernel(up_v, dn_v, recv, up_o, dn_o, mlp_o, total, sem):
    copies = [pltpu.make_async_copy(up_v, up_o, sem.at[0]), pltpu.make_async_copy(dn_v, dn_o, sem.at[1])]
    for c in copies:
        c.start()
    n, T, _ = recv.shape
    rows = 128

    @pl.loop(0, T // rows)
    def _(i):
        r = pl.ds(pl.multiple_of(i * rows, rows), rows)
        acc = recv[0, r, :].astype(jnp.float32)
        for k in range(1, n):
            acc += recv[k, r, :].astype(jnp.float32)
        total[r, :] = acc.astype(jnp.bfloat16)

    last = pltpu.make_async_copy(total, mlp_o, sem.at[2])
    last.start()
    for c in copies:
        c.wait()
    last.wait()


def solution(mesh):
    n_fs, n_tp = mesh.shape["fs"], mesh.shape["tp"]
    bf16 = jnp.bfloat16

    def on_device(tokens, norm_gain, up_master, down_master):
        up_l = (norm_gain[:, None] * up_master).astype(bf16)
        dn_l = jnp.transpose(down_master).astype(bf16)
        T, Dk = tokens.shape
        R, F = up_l.shape
        D = n_fs * R
        W = R // 2 if (R // 2) % 128 == 0 else R
        S = len(send_list(n_fs))
        any_spec = pl.BlockSpec(memory_space=pl.ANY)
        vmem_spec = pl.BlockSpec(memory_space=pltpu.VMEM)
        up_v, dn_v, recv = pl.pallas_call(
            functools.partial(gather_kernel, n_fs, n_tp),
            out_shape=(pltpu.VMEM((D, F), bf16), pltpu.VMEM((F, D), bf16), pltpu.VMEM((n_tp, T, Dk), bf16)),
            in_specs=[any_spec] * 3,
            out_specs=(vmem_spec,) * 3,
            scratch_shapes=[
                pltpu.VMEM((T, D), bf16),
                pltpu.VMEM((T, F), bf16),
                pltpu.VMEM((D // W, T, W), bf16),
                pltpu.SemaphoreType.DMA((3,)),
                pltpu.SemaphoreType.DMA((n_tp,)),
                pltpu.SemaphoreType.DMA((n_tp,)),
                pltpu.SemaphoreType.DMA((2, S)),
                pltpu.SemaphoreType.DMA((2, S)),
                pltpu.SemaphoreType.DMA((D // W,)),
                pltpu.SemaphoreType.DMA((n_tp, Dk // W)),
            ],
            compiler_params=pltpu.CompilerParams(
                collective_id=0, has_side_effects=True, vmem_limit_bytes=30 * 2**20
            ),
        )(tokens, up_l, dn_l)
        return pl.pallas_call(
            finish_kernel,
            out_shape=(
                jax.ShapeDtypeStruct((D, F), bf16),
                jax.ShapeDtypeStruct((F, D), bf16),
                jax.ShapeDtypeStruct((T, Dk), bf16),
            ),
            in_specs=[vmem_spec] * 3,
            out_specs=(any_spec,) * 3,
            scratch_shapes=[pltpu.VMEM((T, Dk), bf16), pltpu.SemaphoreType.DMA((3,))],
            compiler_params=pltpu.CompilerParams(vmem_limit_bytes=8 * 2**20),
        )(up_v, dn_v, recv)

    in_specs = (P("fs", "tp"), P("fs"), P("fs", "tp"), P("fs", "tp"))
    out_specs = (P(None, "tp"), P("tp", None), P("fs", "tp"))
    return jax.shard_map(on_device, mesh=mesh, in_specs=in_specs, out_specs=out_specs, check_vma=False)
```

```python
import functools

import jax
import jax.numpy as jnp
from jax import lax
from jax.experimental import pallas as pl
from jax.experimental.pallas import tpu as pltpu
from jax.sharding import PartitionSpec as P

norm_floor = 1e-06
MESH = pl.DeviceIdType.MESH


def grid_of(n):
    ny = max(d for d in range(1, n + 1) if n % d == 0 and d * d <= n)
    return n // ny, ny


def position_of(f, nz, ny):
    if ny == 1:
        return f
    z, y = lax.div(f, ny), lax.rem(f, ny)
    tail = lax.div(y + (ny - 1), ny)
    k = nz - 1 - z
    odd = lax.rem(k, 2)
    r = (1 - odd) * (y - 1) + odd * (ny - 1 - y)
    return (1 - tail) * z + tail * (nz + k * (ny - 1) + r)


def index_at(p, nz, ny):
    if ny == 1:
        return p
    tail = lax.div(lax.div(p, nz) + (ny - 2), ny - 1)
    q = tail * (p - nz)
    k = lax.div(q, ny - 1)
    r = lax.rem(q, ny - 1)
    odd = lax.rem(k, 2)
    z = (1 - tail) * p + tail * (nz - 1 - k)
    y = tail * ((1 - odd) * (1 + r) + odd * (ny - 1 - r))
    return z * ny + y


def send_list(n):
    hops = n // 2
    split = n % 2 == 0

    def pieces(a, h):
        return [(a, h, 0)] if split and h == hops - 1 else [(a, h, 0), (a, h, 1)]

    ups = [p for h in range(1, hops) for p in pieces("u", h)]
    downs = [p for h in range(1, hops) for p in pieces("d", h)]
    own_u, own_d = pieces("u", 0), pieces("d", 0)
    return own_u + own_d[:1] + ups + own_d[1:] + downs


def gather_kernel(
    n_fs, n_tp, tokens, gain, up_l, dn_l, up_w, dn_w, recv, x, hid, part, stage, up_f, dn_f, gain_v,
    loc_sem, tok_s, tok_r, ring_s, ring_r, pre_s, pre_r, rs_s, rs_r,
):
    nz, ny = grid_of(n_fs)
    me_f, me_t = lax.axis_index("fs"), lax.axis_index("tp")
    pos = position_of(me_f, nz, ny)
    T, Dk = tokens.shape
    R, F = up_l.shape
    D = n_fs * R
    split_cols = (R // 2) % 128 == 0
    W = R // 2 if split_cols else R

    def at(offset):
        return index_at(lax.rem(pos + offset + n_fs, n_fs), nz, ny)

    right, left = at(1), at(-1)

    def tp_peer(k):
        return lax.rem(me_t + k, n_tp)

    barrier = pltpu.get_barrier_semaphore()
    for f in (right, left):
        pl.semaphore_signal(barrier, inc=1, device_id={"fs": f, "tp": me_t}, device_id_type=MESH)
    for k in range(1, n_tp):
        pl.semaphore_signal(barrier, inc=1, device_id={"fs": me_f, "tp": tp_peer(k)}, device_id_type=MESH)

    def up_piece(f, h):
        return up_w.at[pl.ds(pl.multiple_of(f * R + h * (R // 2), R // 2), R // 2), :]

    def dn_piece(f, h):
        if split_cols:
            return dn_w.at[:, pl.ds(pl.multiple_of(f * R + h * (R // 2), R // 2), R // 2)]
        return dn_w.at[pl.ds(h * (F // 2), F // 2), pl.ds(pl.multiple_of(f * R, R), R)]

    def tok_cols(t):
        return x.at[:, pl.ds(pl.multiple_of(t * Dk, Dk), Dk)]

    own = [
        pltpu.make_async_copy(up_l, up_f, loc_sem.at[0]),
        pltpu.make_async_copy(tokens, tok_cols(me_t), loc_sem.at[1]),
        pltpu.make_async_copy(dn_l, dn_f, loc_sem.at[2]),
    ]
    gain_copy = pltpu.make_async_copy(gain, gain_v, loc_sem.at[3])
    for c in [gain_copy] + own:
        c.start()
    own_rows = pl.ds(pl.multiple_of(me_f * R, R), R)
    gain_copy.wait()
    spread = jnp.transpose(jnp.broadcast_to(gain_v[...], (128, R)))
    own[0].wait()
    for c in range(F // 128):
        cols = pl.ds(c * 128, 128)
        up_w[own_rows, cols] = (spread * up_f[:, cols]).astype(jnp.bfloat16)
    own[1].wait()
    pl.semaphore_wait(barrier, n_tp + 1)

    order = send_list(n_fs)
    S = len(order)

    def ring_copy(s, d):
        a, hop, second = order[s]
        half = second if d == 0 else 1 - second
        f = at(-hop if d == 0 else hop)
        ref = up_piece(f, half) if a == "u" else dn_piece(f, half)
        return pltpu.make_async_remote_copy(
            src_ref=ref, dst_ref=ref, send_sem=ring_s.at[d, s], recv_sem=ring_r.at[d, s],
            device_id={"fs": right if d == 0 else left, "tp": me_t}, device_id_type=MESH,
        )

    def arrival(s, d):
        a, hop, second = order[s]
        half = second if d == 0 else 1 - second
        f = at(-(hop + 1) if d == 0 else hop + 1)
        return f, half, (up_piece(f, half) if a == "u" else dn_piece(f, half))

    def wait_arrival(s, d):
        f, half, ref = arrival(s, d)
        pltpu.make_async_remote_copy(
            src_ref=ref, dst_ref=ref, send_sem=ring_s.at[d, s], recv_sem=ring_r.at[d, s],
            device_id={"fs": right if d == 0 else left, "tp": me_t}, device_id_type=MESH,
        ).wait_recv()

    needs = [-1 if hop == 0 else order.index((a, hop - 1, second)) for a, hop, second in order]
    issued = [0]

    def issue(upto):
        while issued[0] < S and needs[issued[0]] <= upto:
            if upto < 0 and issued[0] >= 3:
                break
            for d in range(2):
                ring_copy(issued[0], d).start()
            issued[0] += 1

    for s in range(2):
        for d in range(2):
            ring_copy(s, d).start()

    def token_copy(k):
        return pltpu.make_async_remote_copy(
            src_ref=tok_cols(me_t), dst_ref=tok_cols(me_t), send_sem=tok_s.at[k], recv_sem=tok_r.at[k],
            device_id={"fs": me_f, "tp": tp_peer(k)}, device_id_type=MESH,
        )

    for k in range(1, n_tp):
        token_copy(k).start()
    own[2].wait()
    block = min(F, 256)

    @pl.loop(0, F // block)
    def _(i):
        r = pl.ds(pl.multiple_of(i * block, block), block)
        dn_w[r, own_rows] = jnp.transpose(dn_f[:, r]).astype(jnp.bfloat16)

    issued[0] = 2
    issue(-1)

    def normalise():
        for k in range(1, n_tp):
            src = lax.rem(me_t - k + n_tp, n_tp)
            pltpu.make_async_remote_copy(
                src_ref=tok_cols(src), dst_ref=tok_cols(src), send_sem=tok_s.at[k], recv_sem=tok_r.at[k],
                device_id={"fs": me_f, "tp": tp_peer(k)}, device_id_type=MESH,
            ).wait_recv()
            token_copy(k).wait_send()
        rows = 64

        @pl.loop(0, T // rows)
        def _(i):
            r = pl.ds(pl.multiple_of(i * rows, rows), rows)
            v = x[r, :].astype(jnp.float32)
            x[r, :] = (v * lax.rsqrt(jnp.mean(v * v, axis=-1, keepdims=True) + norm_floor)).astype(jnp.bfloat16)

    def make_hidden():
        width = 256

        @pl.loop(0, F // width)
        def _(i):
            c = pl.ds(pl.multiple_of(i * width, width), width)
            pre = jnp.dot(x[...], up_w[:, c], preferred_element_type=jnp.float32)
            hid[:, c] = jnp.square(jnp.maximum(pre, 0.0)).astype(jnp.bfloat16)

    per_owner = Dk // W
    nx = n_tp // 2
    half_rows = T // 2
    me_x, me_c = lax.div(me_t, 2), lax.rem(me_t, 2)
    sibling = me_t + 1 - 2 * me_c
    my_half = pl.ds(pl.multiple_of(me_c * half_rows, half_rows), half_rows)
    its_half = pl.ds(pl.multiple_of((1 - me_c) * half_rows, half_rows), half_rows)

    def device(t):
        return dict(device_id={"fs": me_f, "tp": t}, device_id_type=MESH)

    def cols_of(q):
        return pl.ds(pl.multiple_of(lax.rem(q, per_owner) * W, W), W)

    def whole_copy(q):
        return pltpu.make_async_remote_copy(
            src_ref=part.at[q], dst_ref=recv.at[nx, :, cols_of(q)],
            send_sem=rs_s.at[q], recv_sem=rs_r.at[nx, lax.rem(q, per_owner), 0], **device(sibling),
        )

    def pair_copy(q):
        return pltpu.make_async_remote_copy(
            src_ref=part.at[q, its_half], dst_ref=stage.at[q],
            send_sem=pre_s.at[q], recv_sem=pre_r.at[q], **device(sibling),
        )

    def half_copy(q):
        return pltpu.make_async_remote_copy(
            src_ref=part.at[q, my_half], dst_ref=recv.at[me_x, my_half, cols_of(q)],
            send_sem=rs_s.at[q], recv_sem=rs_r.at[me_x, lax.rem(q, per_owner), me_c],
            **device(lax.div(q, per_owner)),
        )

    def share(q):
        owner = lax.div(q, per_owner)

        @pl.when(owner == sibling)
        def _():
            whole_copy(q).start()

        @pl.when(lax.div(owner, 2) != me_x)
        def _():
            pair_copy(q).start()

    def pass_on(q):
        @pl.when(lax.div(q, 2 * per_owner) != me_x)
        def _():
            pair_copy(q).wait_recv()
            both = part[q, my_half, :].astype(jnp.float32) + stage[q].astype(jnp.float32)
            part[q, my_half, :] = both.astype(jnp.bfloat16)
            half_copy(q).start()

    def do_parts(first, count):
        c = pl.ds(pl.multiple_of(first * W, W), count * W)

        @pl.loop(0, 2)
        def _(i):
            r = pl.ds(pl.multiple_of(i * half_rows, half_rows), half_rows)
            out = jnp.dot(hid[r, :], dn_w[:, c], preferred_element_type=jnp.float32).astype(jnp.bfloat16)
            for k in range(count):
                part[first + k, r, :] = out[:, k * W : (k + 1) * W]

        for k in range(count):
            share(first + k)

    per_chunk = R // W
    ready = [(me_f * per_chunk, per_chunk)]
    last_up = max(s for s in range(S) if order[s][0] == "u")
    norm_at = max(0, last_up - 2)
    for s in range(S):
        for d in range(2):
            wait_arrival(s, d)
        issue(s)
        a, hop, _ = order[s]
        if a == "d" and split_cols:
            if n_fs % 2 == 0 and hop == n_fs // 2 - 1:
                ready.append((at(hop + 1) * 2, 2))
            else:
                for d in range(2):
                    f, half, _ = arrival(s, d)
                    ready.append((f * 2 + half, 1))
        if s == norm_at:
            normalise()
        if s == last_up:
            make_hidden()
        if s >= last_up:
            for first, count in ready:
                do_parts(first, count)
            for first, count in ready:
                for k in range(count):
                    pass_on(first + k)
            ready = []
    if not split_cols:
        @pl.loop(0, n_fs)
        def _(q):
            @pl.when(q != me_f)
            def _():
                do_parts(q, 1)
                pass_on(q)

    @pl.loop(0, per_owner)
    def _(local):
        cols = pl.ds(pl.multiple_of(local * W, W), W)
        recv[me_x, :, cols] = part[me_t * per_owner + local]

    for d in range(2):
        for s in range(S):
            ring_copy(s, d).wait_send()

    @pl.loop(0, D // W)
    def _(q):
        owner = lax.div(q, per_owner)

        @pl.when(owner == sibling)
        def _():
            whole_copy(q).wait_send()

        @pl.when(lax.div(owner, 2) != me_x)
        def _():
            pair_copy(q).wait_send()
            half_copy(q).wait_send()

    for local in range(per_owner):
        q = me_t * per_owner + local
        whole_copy(q).wait_recv()
        for k in range(1, nx):
            src = lax.rem(me_x + k, nx)
            for c in range(2):
                ref = recv.at[src, pl.ds(c * half_rows, half_rows), pl.ds(local * W, W)]
                pltpu.make_async_remote_copy(
                    src_ref=ref, dst_ref=ref, send_sem=rs_s.at[0], recv_sem=rs_r.at[src, local, c], **device(sibling),
                ).wait_recv()


def finish_kernel(up_v, dn_v, recv, up_o, dn_o, mlp_o, total, sem):
    copies = [pltpu.make_async_copy(up_v, up_o, sem.at[0]), pltpu.make_async_copy(dn_v, dn_o, sem.at[1])]
    for c in copies:
        c.start()
    n, T, _ = recv.shape
    rows = 128

    @pl.loop(0, T // rows)
    def _(i):
        r = pl.ds(pl.multiple_of(i * rows, rows), rows)
        acc = recv[0, r, :].astype(jnp.float32)
        for k in range(1, n):
            acc += recv[k, r, :].astype(jnp.float32)
        total[r, :] = acc.astype(jnp.bfloat16)

    last = pltpu.make_async_copy(total, mlp_o, sem.at[2])
    last.start()
    for c in copies:
        c.wait()
    last.wait()


def solution(mesh):
    n_fs, n_tp = mesh.shape["fs"], mesh.shape["tp"]
    bf16 = jnp.bfloat16

    def on_device(tokens, norm_gain, up_master, down_master):
        T, Dk = tokens.shape
        R, F = up_master.shape
        D = n_fs * R
        W = R // 2 if (R // 2) % 128 == 0 else R
        S = len(send_list(n_fs))
        any_spec = pl.BlockSpec(memory_space=pl.ANY)
        vmem_spec = pl.BlockSpec(memory_space=pltpu.VMEM)
        up_v, dn_v, recv = pl.pallas_call(
            functools.partial(gather_kernel, n_fs, n_tp),
            out_shape=(pltpu.VMEM((D, F), bf16), pltpu.VMEM((F, D), bf16), pltpu.VMEM((n_tp // 2 + 1, T, Dk), bf16)),
            in_specs=[pl.BlockSpec(memory_space=pltpu.HBM)] * 4,
            out_specs=(vmem_spec,) * 3,
            scratch_shapes=[
                pltpu.VMEM((T, D), bf16),
                pltpu.VMEM((T, F), bf16),
                pltpu.VMEM((D // W, T, W), bf16),
                pltpu.VMEM((D // W, T // 2, W), bf16),
                pltpu.VMEM((R, F), jnp.float32),
                pltpu.VMEM((R, F), jnp.float32),
                pltpu.VMEM((1, R), jnp.float32),
                pltpu.SemaphoreType.DMA((4,)),
                pltpu.SemaphoreType.DMA((n_tp,)),
                pltpu.SemaphoreType.DMA((n_tp,)),
                pltpu.SemaphoreType.DMA((2, S)),
                pltpu.SemaphoreType.DMA((2, S)),
                pltpu.SemaphoreType.DMA((D // W,)),
                pltpu.SemaphoreType.DMA((D // W,)),
                pltpu.SemaphoreType.DMA((D // W,)),
                pltpu.SemaphoreType.DMA((n_tp // 2 + 1, Dk // W, 2)),
            ],
            compiler_params=pltpu.CompilerParams(
                collective_id=0, has_side_effects=True, vmem_limit_bytes=44 * 2**20
            ),
        )(tokens, norm_gain[None, :], up_master, down_master)
        return pl.pallas_call(
            finish_kernel,
            out_shape=(
                jax.ShapeDtypeStruct((D, F), bf16),
                jax.ShapeDtypeStruct((F, D), bf16),
                jax.ShapeDtypeStruct((T, Dk), bf16),
            ),
            in_specs=[vmem_spec] * 3,
            out_specs=(any_spec,) * 3,
            scratch_shapes=[pltpu.VMEM((T, Dk), bf16), pltpu.SemaphoreType.DMA((3,))],
            compiler_params=pltpu.CompilerParams(vmem_limit_bytes=8 * 2**20),
        )(up_v, dn_v, recv)

    in_specs = (P("fs", "tp"), P("fs"), P("fs", "tp"), P("fs", "tp"))
    out_specs = (P(None, "tp"), P("tp", None), P("fs", "tp"))
    return jax.shard_map(on_device, mesh=mesh, in_specs=in_specs, out_specs=out_specs, check_vma=False)
```

```python
import functools

import jax
import jax.numpy as jnp
from jax import lax
from jax.experimental import pallas as pl
from jax.experimental.pallas import tpu as pltpu
from jax.sharding import PartitionSpec as P

norm_floor = 1e-06
MESH = pl.DeviceIdType.MESH


def grid_of(n):
    ny = max(d for d in range(1, n + 1) if n % d == 0 and d * d <= n)
    return n // ny, ny


def position_of(f, nz, ny):
    if ny == 1:
        return f
    z, y = lax.div(f, ny), lax.rem(f, ny)
    tail = lax.div(y + (ny - 1), ny)
    k = nz - 1 - z
    odd = lax.rem(k, 2)
    r = (1 - odd) * (y - 1) + odd * (ny - 1 - y)
    return (1 - tail) * z + tail * (nz + k * (ny - 1) + r)


def index_at(p, nz, ny):
    if ny == 1:
        return p
    tail = lax.div(lax.div(p, nz) + (ny - 2), ny - 1)
    q = tail * (p - nz)
    k = lax.div(q, ny - 1)
    r = lax.rem(q, ny - 1)
    odd = lax.rem(k, 2)
    z = (1 - tail) * p + tail * (nz - 1 - k)
    y = tail * ((1 - odd) * (1 + r) + odd * (ny - 1 - r))
    return z * ny + y


def send_list(n):
    hops = n // 2
    split = n % 2 == 0

    def pieces(a, h):
        return [(a, h, 0)] if split and h == hops - 1 else [(a, h, 0), (a, h, 1)]

    ups = [p for h in range(1, hops) for p in pieces("u", h)]
    downs = [p for h in range(1, hops) for p in pieces("d", h)]
    own_u, own_d = pieces("u", 0), pieces("d", 0)
    return own_u + own_d[:1] + ups + own_d[1:] + downs


def gather_kernel(
    n_fs, n_tp, tokens, gain, up_l, dn_l, up_w, dn_w, recv, x, hid, part, stage, up_f, dn_f, gain_v,
    loc_sem, tok_s, tok_r, ring_s, ring_r, pre_s, pre_r, rs_s, rs_r,
):
    nz, ny = grid_of(n_fs)
    me_f, me_t = lax.axis_index("fs"), lax.axis_index("tp")
    pos = position_of(me_f, nz, ny)
    T, Dk = tokens.shape
    R, F = up_l.shape
    D = n_fs * R
    split_cols = (R // 2) % 128 == 0
    W = R // 2 if split_cols else R

    def at(offset):
        return index_at(lax.rem(pos + offset + n_fs, n_fs), nz, ny)

    right, left = at(1), at(-1)

    def tp_peer(k):
        return lax.rem(me_t + k, n_tp)

    barrier = pltpu.get_barrier_semaphore()
    for f in (right, left):
        pl.semaphore_signal(barrier, inc=1, device_id={"fs": f, "tp": me_t}, device_id_type=MESH)
    for k in range(1, n_tp):
        pl.semaphore_signal(barrier, inc=1, device_id={"fs": me_f, "tp": tp_peer(k)}, device_id_type=MESH)

    def up_piece(f, h):
        return up_w.at[pl.ds(pl.multiple_of(f * R + h * (R // 2), R // 2), R // 2), :]

    def dn_piece(f, h):
        if split_cols:
            return dn_w.at[:, pl.ds(pl.multiple_of(f * R + h * (R // 2), R // 2), R // 2)]
        return dn_w.at[pl.ds(h * (F // 2), F // 2), pl.ds(pl.multiple_of(f * R, R), R)]

    def tok_cols(t):
        return x.at[:, pl.ds(pl.multiple_of(t * Dk, Dk), Dk)]

    own = [
        pltpu.make_async_copy(up_l, up_f, loc_sem.at[0]),
        pltpu.make_async_copy(tokens, tok_cols(me_t), loc_sem.at[1]),
        pltpu.make_async_copy(dn_l, dn_f, loc_sem.at[2]),
    ]
    gain_copy = pltpu.make_async_copy(gain, gain_v, loc_sem.at[3])
    for c in [gain_copy] + own:
        c.start()
    own_rows = pl.ds(pl.multiple_of(me_f * R, R), R)
    gain_copy.wait()
    spread = jnp.transpose(jnp.broadcast_to(gain_v[...], (128, R)))
    own[0].wait()
    for c in range(F // 128):
        cols = pl.ds(c * 128, 128)
        up_w[own_rows, cols] = (spread * up_f[:, cols]).astype(jnp.bfloat16)
    own[1].wait()
    pl.semaphore_wait(barrier, n_tp + 1)

    order = send_list(n_fs)
    S = len(order)

    def ring_copy(s, d):
        a, hop, second = order[s]
        half = second if d == 0 else 1 - second
        f = at(-hop if d == 0 else hop)
        ref = up_piece(f, half) if a == "u" else dn_piece(f, half)
        return pltpu.make_async_remote_copy(
            src_ref=ref, dst_ref=ref, send_sem=ring_s.at[d, s], recv_sem=ring_r.at[d, s],
            device_id={"fs": right if d == 0 else left, "tp": me_t}, device_id_type=MESH,
        )

    def arrival(s, d):
        a, hop, second = order[s]
        half = second if d == 0 else 1 - second
        f = at(-(hop + 1) if d == 0 else hop + 1)
        return f, half, (up_piece(f, half) if a == "u" else dn_piece(f, half))

    def wait_arrival(s, d):
        f, half, ref = arrival(s, d)
        pltpu.make_async_remote_copy(
            src_ref=ref, dst_ref=ref, send_sem=ring_s.at[d, s], recv_sem=ring_r.at[d, s],
            device_id={"fs": right if d == 0 else left, "tp": me_t}, device_id_type=MESH,
        ).wait_recv()

    needs = [-1 if hop == 0 else order.index((a, hop - 1, second)) for a, hop, second in order]
    issued = [0]

    def issue(upto):
        while issued[0] < S and needs[issued[0]] <= upto:
            if upto < 0 and issued[0] >= 3:
                break
            for d in range(2):
                ring_copy(issued[0], d).start()
            issued[0] += 1

    for s in range(2):
        for d in range(2):
            ring_copy(s, d).start()

    def token_copy(k):
        return pltpu.make_async_remote_copy(
            src_ref=tok_cols(me_t), dst_ref=tok_cols(me_t), send_sem=tok_s.at[k], recv_sem=tok_r.at[k],
            device_id={"fs": me_f, "tp": tp_peer(k)}, device_id_type=MESH,
        )

    for k in range(1, n_tp):
        token_copy(k).start()
    own[2].wait()
    block = min(F, 256)

    @pl.loop(0, F // block)
    def _(i):
        r = pl.ds(pl.multiple_of(i * block, block), block)
        dn_w[r, own_rows] = jnp.transpose(dn_f[:, r]).astype(jnp.bfloat16)

    issued[0] = 2
    issue(-1)

    def normalise():
        for k in range(1, n_tp):
            src = lax.rem(me_t - k + n_tp, n_tp)
            pltpu.make_async_remote_copy(
                src_ref=tok_cols(src), dst_ref=tok_cols(src), send_sem=tok_s.at[k], recv_sem=tok_r.at[k],
                device_id={"fs": me_f, "tp": tp_peer(k)}, device_id_type=MESH,
            ).wait_recv()
            token_copy(k).wait_send()
        rows = 64

        @pl.loop(0, T // rows)
        def _(i):
            r = pl.ds(pl.multiple_of(i * rows, rows), rows)
            v = x[r, :].astype(jnp.float32)
            x[r, :] = (v * lax.rsqrt(jnp.mean(v * v, axis=-1, keepdims=True) + norm_floor)).astype(jnp.bfloat16)

    def make_hidden():
        width = 256

        @pl.loop(0, F // width)
        def _(i):
            c = pl.ds(pl.multiple_of(i * width, width), width)
            pre = jnp.dot(x[...], up_w[:, c], preferred_element_type=jnp.float32)
            hid[:, c] = jnp.square(jnp.maximum(pre, 0.0)).astype(jnp.bfloat16)

    per_owner = Dk // W
    nx = n_tp // 2
    half_rows = T // 2
    me_x, me_c = lax.div(me_t, 2), lax.rem(me_t, 2)
    sibling = me_t + 1 - 2 * me_c
    my_half = pl.ds(pl.multiple_of(me_c * half_rows, half_rows), half_rows)
    its_half = pl.ds(pl.multiple_of((1 - me_c) * half_rows, half_rows), half_rows)

    def device(t):
        return dict(device_id={"fs": me_f, "tp": t}, device_id_type=MESH)

    def cols_of(q):
        return pl.ds(pl.multiple_of(lax.rem(q, per_owner) * W, W), W)

    def whole_copy(q):
        return pltpu.make_async_remote_copy(
            src_ref=part.at[q], dst_ref=recv.at[nx, :, cols_of(q)],
            send_sem=rs_s.at[q], recv_sem=rs_r.at[nx, lax.rem(q, per_owner), 0], **device(sibling),
        )

    def pair_copy(q):
        return pltpu.make_async_remote_copy(
            src_ref=part.at[q, its_half], dst_ref=stage.at[q],
            send_sem=pre_s.at[q], recv_sem=pre_r.at[q], **device(sibling),
        )

    def half_copy(q):
        return pltpu.make_async_remote_copy(
            src_ref=part.at[q, my_half], dst_ref=recv.at[me_x, my_half, cols_of(q)],
            send_sem=rs_s.at[q], recv_sem=rs_r.at[me_x, lax.rem(q, per_owner), me_c],
            **device(lax.div(q, per_owner)),
        )

    def pass_on(q):
        @pl.when(lax.div(q, 2 * per_owner) != me_x)
        def _():
            pair_copy(q).wait_recv()
            both = part[q, my_half, :].astype(jnp.float32) + stage[q].astype(jnp.float32)
            part[q, my_half, :] = both.astype(jnp.bfloat16)
            half_copy(q).start()

    def do_parts(first, count):
        c = pl.ds(pl.multiple_of(first * W, W), count * W)

        @pl.loop(0, 2)
        def _(i):
            r = pl.ds(pl.multiple_of(lax.rem(i + 1 + me_c, 2) * half_rows, half_rows), half_rows)
            out = jnp.dot(hid[r, :], dn_w[:, c], preferred_element_type=jnp.float32).astype(jnp.bfloat16)
            for k in range(count):
                part[first + k, r, :] = out[:, k * W : (k + 1) * W]
            for k in range(count):
                owner = lax.div(first + k, per_owner)

                @pl.when((i == 0) & (lax.div(owner, 2) != me_x))
                def _():
                    pair_copy(first + k).start()

                @pl.when((i == 1) & (owner == sibling))
                def _():
                    whole_copy(first + k).start()

    per_chunk = R // W
    ready = [(me_f * per_chunk, per_chunk)]
    last_up = max(s for s in range(S) if order[s][0] == "u")
    norm_at = max(0, last_up - 2)
    for s in range(S):
        for d in range(2):
            wait_arrival(s, d)
        issue(s)
        a, hop, _ = order[s]
        if a == "d" and split_cols:
            if n_fs % 2 == 0 and hop == n_fs // 2 - 1:
                ready.append((at(hop + 1) * 2, 2))
            else:
                for d in range(2):
                    f, half, _ = arrival(s, d)
                    ready.append((f * 2 + half, 1))
        if s == norm_at:
            normalise()
        if s == last_up:
            make_hidden()
        if s >= last_up:
            for first, count in ready:
                do_parts(first, count)
            for first, count in ready:
                for k in range(count):
                    pass_on(first + k)
            ready = []
    if not split_cols:
        @pl.loop(0, n_fs)
        def _(q):
            @pl.when(q != me_f)
            def _():
                do_parts(q, 1)
                pass_on(q)

    @pl.loop(0, per_owner)
    def _(local):
        cols = pl.ds(pl.multiple_of(local * W, W), W)
        recv[me_x, :, cols] = part[me_t * per_owner + local]

    for d in range(2):
        for s in range(S):
            ring_copy(s, d).wait_send()

    @pl.loop(0, D // W)
    def _(q):
        owner = lax.div(q, per_owner)

        @pl.when(owner == sibling)
        def _():
            whole_copy(q).wait_send()

        @pl.when(lax.div(owner, 2) != me_x)
        def _():
            pair_copy(q).wait_send()
            half_copy(q).wait_send()

    for local in range(per_owner):
        q = me_t * per_owner + local
        whole_copy(q).wait_recv()
        for k in range(1, nx):
            src = lax.rem(me_x + k, nx)
            for c in range(2):
                ref = recv.at[src, pl.ds(c * half_rows, half_rows), pl.ds(local * W, W)]
                pltpu.make_async_remote_copy(
                    src_ref=ref, dst_ref=ref, send_sem=rs_s.at[0], recv_sem=rs_r.at[src, local, c], **device(sibling),
                ).wait_recv()


def finish_kernel(up_v, dn_v, recv, up_o, dn_o, mlp_o, total, sem):
    copies = [pltpu.make_async_copy(up_v, up_o, sem.at[0]), pltpu.make_async_copy(dn_v, dn_o, sem.at[1])]
    for c in copies:
        c.start()
    n, T, _ = recv.shape
    rows = 128

    @pl.loop(0, T // rows)
    def _(i):
        r = pl.ds(pl.multiple_of(i * rows, rows), rows)
        acc = recv[0, r, :].astype(jnp.float32)
        for k in range(1, n):
            acc += recv[k, r, :].astype(jnp.float32)
        total[r, :] = acc.astype(jnp.bfloat16)

    last = pltpu.make_async_copy(total, mlp_o, sem.at[2])
    last.start()
    for c in copies:
        c.wait()
    last.wait()


def solution(mesh):
    n_fs, n_tp = mesh.shape["fs"], mesh.shape["tp"]
    bf16 = jnp.bfloat16

    def on_device(tokens, norm_gain, up_master, down_master):
        T, Dk = tokens.shape
        R, F = up_master.shape
        D = n_fs * R
        W = R // 2 if (R // 2) % 128 == 0 else R
        S = len(send_list(n_fs))
        any_spec = pl.BlockSpec(memory_space=pl.ANY)
        vmem_spec = pl.BlockSpec(memory_space=pltpu.VMEM)
        up_v, dn_v, recv = pl.pallas_call(
            functools.partial(gather_kernel, n_fs, n_tp),
            out_shape=(pltpu.VMEM((D, F), bf16), pltpu.VMEM((F, D), bf16), pltpu.VMEM((n_tp // 2 + 1, T, Dk), bf16)),
            in_specs=[pl.BlockSpec(memory_space=pltpu.HBM)] * 4,
            out_specs=(vmem_spec,) * 3,
            scratch_shapes=[
                pltpu.VMEM((T, D), bf16),
                pltpu.VMEM((T, F), bf16),
                pltpu.VMEM((D // W, T, W), bf16),
                pltpu.VMEM((D // W, T // 2, W), bf16),
                pltpu.VMEM((R, F), jnp.float32),
                pltpu.VMEM((R, F), jnp.float32),
                pltpu.VMEM((1, R), jnp.float32),
                pltpu.SemaphoreType.DMA((4,)),
                pltpu.SemaphoreType.DMA((n_tp,)),
                pltpu.SemaphoreType.DMA((n_tp,)),
                pltpu.SemaphoreType.DMA((2, S)),
                pltpu.SemaphoreType.DMA((2, S)),
                pltpu.SemaphoreType.DMA((D // W,)),
                pltpu.SemaphoreType.DMA((D // W,)),
                pltpu.SemaphoreType.DMA((D // W,)),
                pltpu.SemaphoreType.DMA((n_tp // 2 + 1, Dk // W, 2)),
            ],
            compiler_params=pltpu.CompilerParams(
                collective_id=0, has_side_effects=True, vmem_limit_bytes=44 * 2**20
            ),
        )(tokens, norm_gain[None, :], up_master, down_master)
        return pl.pallas_call(
            finish_kernel,
            out_shape=(
                jax.ShapeDtypeStruct((D, F), bf16),
                jax.ShapeDtypeStruct((F, D), bf16),
                jax.ShapeDtypeStruct((T, Dk), bf16),
            ),
            in_specs=[vmem_spec] * 3,
            out_specs=(any_spec,) * 3,
            scratch_shapes=[pltpu.VMEM((T, Dk), bf16), pltpu.SemaphoreType.DMA((3,))],
            compiler_params=pltpu.CompilerParams(vmem_limit_bytes=8 * 2**20),
        )(up_v, dn_v, recv)

    in_specs = (P("fs", "tp"), P("fs"), P("fs", "tp"), P("fs", "tp"))
    out_specs = (P(None, "tp"), P("tp", None), P("fs", "tp"))
    return jax.shard_map(on_device, mesh=mesh, in_specs=in_specs, out_specs=out_specs, check_vma=False)
```
